32 devices in a mesh: sp: 16 (over z, y, x), tp: 2 (over core).
Axes of the slice: x: 2, y: 2, z: 4, core: 2. Of those that a mesh axis runs over, the one named last changes fastest.
Arguments:
- tokens: bfloat16 [2048, 4096], P('sp'), may hold values from -6 to 6
- norm_gain: bfloat16 [4096], replicated, may hold values from 0.099609375 to 1.8984375
- w_pool_in: bfloat16 [4096, 1024], P('sp', 'tp'), may hold values from -0.09375 to 0.09375
- w_x: bfloat16 [4096, 2048], P('sp', 'tp'), may hold values from -0.09375 to 0.09375
- w_z: bfloat16 [4096, 2048], P('sp', 'tp'), may hold values from -0.09375 to 0.09375
- w_b: bfloat16 [4096, 1024], P('sp', 'tp'), may hold values from -0.09375 to 0.09375
- w_c: bfloat16 [4096, 1024], P('sp', 'tp'), may hold values from -0.09375 to 0.09375
- w_dt: bfloat16 [4096, 2, 32], P(None, None, 'tp'), may hold values from -0.09375 to 0.09375
- conv_x: bfloat16 [3, 2048], P(None, 'tp'), may hold values from -3.5 to 3.5
- conv_b: bfloat16 [3, 1024], P(None, 'tp'), may hold values from -3.5 to 3.5
- output_map_taps: bfloat16 [3, 1024], P(None, 'tp'), may hold values from -3.5 to 3.5
- decay_log: float32 [2, 32], P(None, 'tp'), may hold values from -16 to 0
- leak: float32 [2048, 2, 32], P('sp', None, 'tp'), may hold values from 0 to 2
- init_state: float32 [2, 32, 64, 128], P(None, 'tp'), may hold values from -81.4587 to 81.4587
- head_gain: bfloat16 [2048], P('tp'), may hold values from 0.099609375 to 1.8984375
- w_out: bfloat16 [3072, 4096], P('sp', 'tp'), may hold values from -0.109375 to 0.109375
Outputs:
- mixed: bfloat16 [2048, 4096], P('sp', 'tp')
The draws below stay inside these ranges and needn't reach their ends.
All inputs are finite; a program needn't handle non-finite values.
Results may differ from the reference program's by a relative error of at most 0.01.
Values may be sent and summed in bfloat16 or wider, within the bound.
A program may use at most 128 MiB of HBM per device.

```python
import math
import jax
import jax.numpy as jnp
from jax import lax

D = 4096
POOL_W = 1024
POOL_GW = 256
SSD_W = 2048
MIXER_HEAD_SIZE = 64
HEADS = 32
GROUPS = 8
STATE = 128
BLOCK = 128
TOK_DEV = 128
TOKENS = 2048


def draw_decay_log(key, part):
    pick_key, fast_key, slow_key = jax.random.split(jax.random.fold_in(key, 11), 3)
    fast_share = 0.5
    is_fast = jax.random.uniform(pick_key, (2, HEADS), jnp.float32) < fast_share
    fast_rate = jax.random.uniform(fast_key, (2, HEADS), jnp.float32, math.log(0.02), math.log(0.06))
    slow_rate = jax.random.uniform(slow_key, (2, HEADS), jnp.float32, math.log(0.1), math.log(0.4)) - math.log(TOKENS)
    return jnp.where(is_fast, fast_rate, slow_rate)


def draw_leak(key, part):
    level_key, spot_key, size_key = jax.random.split(jax.random.fold_in(key, 23), 3)
    block_count = TOKENS // TOK_DEV
    level = jnp.exp(jax.random.uniform(level_key, (block_count, 2, HEADS), jnp.float32, math.log(0.1), math.log(0.4))) / TOKENS
    starting_shift = jnp.repeat(level, TOK_DEV, axis=0)
    probe_locations = jax.random.randint(spot_key, (2, 2, HEADS), 0, TOKENS)
    overall_quantity = -jnp.log(1.0 - jax.random.uniform(size_key, (2, 2, HEADS), jnp.float32, 0.2, 0.5))
    element_index = jnp.arange(TOKENS, dtype=jnp.int32)[:, None, None, None]
    cluster_sets = jnp.sum(jnp.where(element_index == probe_locations[None], overall_quantity[None], 0.0), axis=1)
    return (starting_shift + cluster_sets).astype(jnp.float32)


def levels(rng, dims, cuts, low, top_value):
    def one(dim, blocks):
        steps = jax.random.uniform(jax.random.fold_in(jax.random.fold_in(rng, 6), dim), (blocks,), jnp.float32, low / len(cuts), top_value / len(cuts))
        return jnp.repeat(jnp.exp(steps), dims[dim] // blocks).reshape((-1,) + (1,) * (len(dims) - dim - 1))

    level = one(*cuts[0])
    for cut in cuts[1:]:
        level = level * one(*cut)
    return level


def noise(rng, dims, spread, limit, pieces=(), kind=jnp.bfloat16):
    values = spread * jax.random.normal(rng, dims, jnp.float32)
    if pieces:
        values = values * levels(rng, dims, pieces, -0.22, 0.18)
    return jnp.clip(values, -limit, limit).astype(kind)


def setup_inputs(seed: int = 0) -> dict:
    key_list = jax.random.split(jax.random.key(seed), 17)
    tokens = noise(key_list[0], (TOKENS, D), 1.0, 6.0, ((0, 16),))
    norm_gain = jnp.clip(1.0 + 0.18 * jax.random.normal(key_list[1], (D,), jnp.float32), 0.099609375, 1.8984375).astype(jnp.bfloat16)
    w_pool_in = noise(key_list[2], (D, POOL_W), D ** -0.5, 0.09375, ((0, 16), (1, 2)))
    w_x = noise(key_list[3], (D, SSD_W), D ** -0.5, 0.09375, ((0, 16), (1, 2)))
    w_z = noise(key_list[4], (D, SSD_W), D ** -0.5, 0.09375, ((0, 16), (1, 2)))
    w_b = noise(key_list[5], (D, GROUPS * STATE), D ** -0.5, 0.09375, ((0, 16), (1, 2)))
    w_c = noise(key_list[6], (D, GROUPS * STATE), D ** -0.5, 0.09375, ((0, 16), (1, 2)))
    w_dt = noise(key_list[7], (D, 2, HEADS), D ** -0.5, 0.09375, ((2, 2),))
    conv_x = noise(key_list[8], (3, SSD_W), 3 ** -0.5, 3.5, ((1, 2),))
    conv_b = noise(key_list[9], (3, GROUPS * STATE), 3 ** -0.5, 3.5, ((1, 2),))
    output_map_taps = noise(key_list[10], (3, GROUPS * STATE), 3 ** -0.5, 3.5, ((1, 2),))
    decay_log = draw_decay_log(jax.random.fold_in(key_list[16], 71), 0)
    leak = draw_leak(jax.random.fold_in(key_list[16], 71), 0)
    init_state = noise(key_list[13], (2, HEADS, MIXER_HEAD_SIZE, STATE), (0.3 * TOKENS ** 0.5), 81.4587, ((1, 2),), jnp.float32)
    head_gain = jnp.clip(1.0 + 0.18 * jax.random.normal(key_list[14], (SSD_W,), jnp.float32), 0.099609375, 1.8984375).astype(jnp.bfloat16)
    w_out = noise(key_list[15], (POOL_W + SSD_W, D), (POOL_W + SSD_W) ** -0.5, 0.109375, ((0, 16), (1, 2)))
    return dict(tokens=tokens, norm_gain=norm_gain, w_pool_in=w_pool_in, w_x=w_x, w_z=w_z, w_b=w_b, w_c=w_c, w_dt=w_dt, conv_x=conv_x, conv_b=conv_b, output_map_taps=output_map_taps, decay_log=decay_log, leak=leak, init_state=init_state, head_gain=head_gain, w_out=w_out)


epsilon = 1e-06
windows = (2, 4, 8, 16)
pool_reach = 8

def rounded(value):
    return lax.optimization_barrier(value.astype(jnp.bfloat16))

def window_means(padded, first_pos, seq_total, channel_group):
    count_rows = padded.shape[0] - 2 * pool_reach
    prefix = jnp.concatenate([jnp.zeros((1, padded.shape[1]), jnp.float32), jnp.cumsum(padded, axis=0)], axis=0)
    element_index = first_pos + jnp.arange(count_rows, dtype=jnp.int32)
    result = jnp.zeros((count_rows, padded.shape[1]), jnp.float32)
    for group_id, window in enumerate(windows):
        low_reach = window // 2
        high_reach = window - 1 - low_reach
        upper_sum = prefix[pool_reach + high_reach + 1:pool_reach + high_reach + 1 + count_rows]
        lower_sum = prefix[pool_reach - low_reach:pool_reach - low_reach + count_rows]
        tallied_items = jnp.minimum(element_index + high_reach, seq_total - 1) - jnp.maximum(element_index - low_reach, 0) + 1
        means = (upper_sum - lower_sum) / tallied_items.astype(jnp.float32)[:, None]
        result = jnp.where(channel_group[None, :] == group_id, means, result)
    return result

def conv_silu(extended, conv_weight):
    weight = conv_weight.astype(jnp.float32)
    values = extended.astype(jnp.float32)
    summed = values[:-2] * weight[0] + values[1:-1] * weight[1] + values[2:] * weight[2]
    return jax.nn.silu(summed)

def ssd_block(state_in, inputs):
    x_blk, b_blk, c_blk, dt_blk, decay_blk = inputs
    block_length = x_blk.shape[0]
    cumul = jnp.cumsum(decay_blk, axis=0)
    scores = jnp.einsum('ign,kgn->gik', c_blk.astype(jnp.float32), b_blk.astype(jnp.float32))
    index = jnp.arange(block_length)
    below = index[:, None] >= index[None, :]
    cumul_t = jnp.transpose(cumul, (1, 2, 0))
    gap_log = cumul_t[:, :, :, None] - cumul_t[:, :, None, :]
    decay_mat = jnp.exp(jnp.where(below, gap_log, -jnp.inf))
    dt_t = jnp.transpose(dt_blk, (1, 2, 0))
    mixing = rounded(scores[:, None] * decay_mat * dt_t[:, :, None, :])
    inner = jnp.einsum('gjik,kgjp->igjp', mixing.astype(jnp.float32), x_blk.astype(jnp.float32))
    carried = jnp.exp(cumul)[..., None] * jnp.einsum('ign,gjpn->igjp', c_blk.astype(jnp.float32), state_in, precision=lax.Precision.HIGHEST)
    to_end = jnp.exp(cumul[-1:] - cumul) * dt_blk
    scaled_b = rounded(to_end[..., None] * b_blk.astype(jnp.float32)[:, :, None, :])
    state_out = jnp.exp(cumul[-1])[..., None, None] * state_in + jnp.einsum('kgjp,kgjn->gjpn', x_blk.astype(jnp.float32), scaled_b.astype(jnp.float32))
    return (state_out, inner + carried)

def run_direction(heads_x, b_groups, c_groups, step_dir, decay_dir, start_state):
    block_count = heads_x.shape[0] // BLOCK

    def to_blocks(values_in):
        return values_in.reshape((block_count, BLOCK) + values_in.shape[1:])
    final_state, outputs = lax.scan(ssd_block, start_state, (to_blocks(heads_x), to_blocks(b_groups), to_blocks(c_groups), to_blocks(step_dir), to_blocks(decay_dir)))
    return outputs.reshape(heads_x.shape)

def reference(tokens, norm_gain, w_pool_in, w_x, w_z, w_b, w_c, w_dt, conv_x, conv_b, output_map_taps, decay_log, leak, init_state, head_gain, w_out):
    seq_total = tokens.shape[0]
    token_f = tokens.astype(jnp.float32)
    normed = rounded(token_f * lax.rsqrt(lax.optimization_barrier(jnp.mean(token_f * token_f, axis=1, keepdims=True)) + epsilon) * norm_gain.astype(jnp.float32))

    def project(weight):
        return jnp.dot(normed, weight, preferred_element_type=jnp.float32)
    pool_in = rounded(project(w_pool_in))
    ssd_x = rounded(project(w_x))
    gate_z = rounded(project(w_z))
    ssd_b = rounded(project(w_b))
    ssd_c = rounded(project(w_c))
    dt_raw = project(w_dt.reshape(w_dt.shape[0], 2 * HEADS)).reshape(seq_total, 2, HEADS)
    channel_group = jnp.arange(POOL_W, dtype=jnp.int32) // POOL_GW
    padded = jnp.pad(pool_in.astype(jnp.float32), ((pool_reach, pool_reach), (0, 0)))
    pooled = rounded(window_means(padded, 0, seq_total, channel_group) - pool_in.astype(jnp.float32))
    stacked = jnp.concatenate([ssd_x, ssd_b, ssd_c], axis=1)
    conv_weight = jnp.concatenate([conv_x, conv_b, output_map_taps], axis=1)
    convolved = rounded(conv_silu(jnp.pad(stacked, ((1, 1), (0, 0))), conv_weight))
    per_group = HEADS // GROUPS
    heads_x = convolved[:, :SSD_W].reshape(seq_total, GROUPS, per_group, MIXER_HEAD_SIZE)
    b_groups = convolved[:, SSD_W:SSD_W + GROUPS * STATE].reshape(seq_total, GROUPS, STATE)
    c_groups = convolved[:, SSD_W + GROUPS * STATE:].reshape(seq_total, GROUPS, STATE)
    step_size = jax.nn.softplus(dt_raw)
    log_decay = -step_size * jnp.exp(decay_log)[None] - leak
    step_size = step_size.reshape(seq_total, 2, GROUPS, per_group)
    log_decay = log_decay.reshape(seq_total, 2, GROUPS, per_group)
    start = init_state.reshape(2, GROUPS, per_group, MIXER_HEAD_SIZE, STATE)
    forward = run_direction(heads_x, b_groups, c_groups, step_size[:, 0], log_decay[:, 0], start[0])
    backward = run_direction(heads_x[::-1], b_groups[::-1], c_groups[::-1], step_size[::-1, 1], log_decay[::-1, 1], start[1])[::-1]
    gated = (forward + backward).reshape(seq_total, HEADS, MIXER_HEAD_SIZE) * jax.nn.silu(gate_z.astype(jnp.float32)).reshape(seq_total, HEADS, MIXER_HEAD_SIZE)
    head_norm = gated * lax.rsqrt(lax.optimization_barrier(jnp.mean(gated * gated, axis=2, keepdims=True)) + epsilon)
    ssd_y = rounded(head_norm.reshape(seq_total, SSD_W) * head_gain.astype(jnp.float32))
    joined = jnp.concatenate([pooled, ssd_y], axis=1)
    return jnp.dot(joined, w_out, preferred_element_type=jnp.float32).astype(jnp.bfloat16)
```

```python
import jax
import jax.numpy as jnp
from jax import lax
from jax.sharding import PartitionSpec as P

POOL_GW = 256
MIXER_HEAD_SIZE = 64
STATE = 128
BLOCK = 128


epsilon = 1e-06
windows = (2, 4, 8, 16)
pool_reach = 8


def with_halo(cells, sides, width):
    for axis, dim in sides:
        count = lax.axis_size(axis)
        ends = count - 1
        head = lax.slice_in_dim(cells, 0, width, axis=dim)
        tail = lax.slice_in_dim(cells, cells.shape[dim] - width, cells.shape[dim], axis=dim)
        cells = jnp.concatenate(
            [
                lax.ppermute(tail, axis, [(i, (i + 1) % count) for i in range(ends)]),
                cells,
                lax.ppermute(head, axis, [((i + 1) % count, i) for i in range(ends)]),
            ],
            axis=dim,
        )
    return cells


def entering(value, axis, combine, identity, reverse):
    length, mine = (lax.axis_size(axis), lax.axis_index(axis))
    everything = jax.tree.map(
        lambda part, kind: lax.all_gather(part.astype(kind), axis),
        value,
        (jnp.bfloat16, jnp.bfloat16),
    )
    start = jax.tree.map(
        lambda part, zero: jnp.broadcast_to(jnp.asarray(zero, part.dtype), part.shape),
        value,
        identity,
    )

    def lap(k, before):
        at = length - 1 - k if reverse else k
        reached = at > mine if reverse else at < mine
        new = combine(
            before, jax.tree.map(lambda part, own: part[at].astype(own.dtype), everything, value)
        )
        return jax.tree.map(lambda a, b: jnp.where(reached, a, b), new, before)

    return lax.fori_loop(0, length, lap, start)


def rounded(value):
    return lax.optimization_barrier(value.astype(jnp.bfloat16))


def window_means(padded, first_pos, seq_total, channel_group):
    count_rows = padded.shape[0] - 2 * pool_reach
    prefix = jnp.concatenate(
        [jnp.zeros((1, padded.shape[1]), jnp.float32), jnp.cumsum(padded, axis=0)], axis=0
    )
    element_index = first_pos + jnp.arange(count_rows, dtype=jnp.int32)
    result = jnp.zeros((count_rows, padded.shape[1]), jnp.float32)
    for group_id, window in enumerate(windows):
        low_reach = window // 2
        high_reach = window - 1 - low_reach
        upper_sum = prefix[pool_reach + high_reach + 1 : pool_reach + high_reach + 1 + count_rows]
        lower_sum = prefix[pool_reach - low_reach : pool_reach - low_reach + count_rows]
        tallied_items = (
            jnp.minimum(element_index + high_reach, seq_total - 1)
            - jnp.maximum(element_index - low_reach, 0)
            + 1
        )
        means = (upper_sum - lower_sum) / tallied_items.astype(jnp.float32)[:, None]
        result = jnp.where(channel_group[None, :] == group_id, means, result)
    return result


def conv_silu(extended, conv_weight):
    weight = conv_weight.astype(jnp.float32)
    values = extended.astype(jnp.float32)
    summed = values[:-2] * weight[0] + values[1:-1] * weight[1] + values[2:] * weight[2]
    return jax.nn.silu(summed)


def ssd_block(state_in, inputs):
    x_blk, b_blk, c_blk, dt_blk, decay_blk = inputs
    block_length = x_blk.shape[0]
    cumul = jnp.cumsum(decay_blk, axis=0)
    scores = jnp.einsum("ign,kgn->gik", c_blk, b_blk, preferred_element_type=jnp.float32)
    index = jnp.arange(block_length)
    below = index[:, None] >= index[None, :]
    cumul_t = jnp.transpose(cumul, (1, 2, 0))
    gap_log = cumul_t[:, :, :, None] - cumul_t[:, :, None, :]
    decay_mat = jnp.exp(jnp.where(below, gap_log, -jnp.inf))
    dt_t = jnp.transpose(dt_blk, (1, 2, 0))
    mixing = (scores[:, None] * decay_mat * dt_t[:, :, None, :]).astype(jnp.bfloat16)
    inner = jnp.einsum("gjik,kgjp->igjp", mixing, x_blk, preferred_element_type=jnp.float32)
    carried = jnp.exp(cumul)[..., None] * jnp.einsum(
        "ign,gjpn->igjp", c_blk.astype(jnp.float32), state_in, precision=lax.Precision.HIGHEST
    )
    to_end = jnp.exp(cumul[-1:] - cumul) * dt_blk
    scaled_b = (to_end[..., None] * b_blk.astype(jnp.float32)[:, :, None, :]).astype(jnp.bfloat16)
    state_out = jnp.exp(cumul[-1])[..., None, None] * state_in + jnp.einsum(
        "kgjp,kgjn->gjpn", x_blk, scaled_b, preferred_element_type=jnp.float32
    )
    return (state_out, inner + carried)


def nearby_orientation(heads_x, b_groups, c_groups, step_dir, decay_dir):
    block_count = heads_x.shape[0] // BLOCK

    def to_blocks(values_in):
        return values_in.reshape((block_count, BLOCK) + values_in.shape[1:])

    zero_state = jnp.zeros(
        (heads_x.shape[1], heads_x.shape[2], heads_x.shape[3], b_groups.shape[2]), jnp.float32
    )
    final_state, outputs = lax.scan(
        ssd_block,
        zero_state,
        (
            to_blocks(heads_x),
            to_blocks(b_groups),
            to_blocks(c_groups),
            to_blocks(step_dir),
            to_blocks(decay_dir),
        ),
    )
    cumul_span = jnp.cumsum(decay_dir, axis=0)
    return (outputs.reshape(heads_x.shape), final_state, jnp.exp(cumul_span[-1]), cumul_span)


def combine_states(earlier, later):
    return (earlier[0] * later[0], earlier[1] * later[0][..., None, None] + later[1])


def including_element(local_out, c_groups, cumul_span, entry):
    return local_out + jnp.exp(cumul_span)[..., None] * jnp.einsum(
        "tgn,gjpn->tgjp", c_groups.astype(jnp.float32), entry, precision=lax.Precision.HIGHEST
    )


def per_device(
    tokens,
    norm_gain,
    w_pool_in,
    w_x,
    w_z,
    w_b,
    w_c,
    w_dt,
    conv_x,
    conv_b,
    output_map_taps,
    decay_log,
    leak,
    init_state,
    head_gain,
    w_out,
):
    tok_rows = tokens.shape[0]
    token_f = tokens.astype(jnp.float32)
    normed = (
        token_f
        * lax.rsqrt(jnp.mean(token_f * token_f, axis=1, keepdims=True) + epsilon)
        * norm_gain.astype(jnp.float32)
    ).astype(jnp.bfloat16)
    w_pieces = (
        lax.all_gather(w_pool_in, "sp", axis=0, tiled=True),
        lax.all_gather(w_x, "sp", axis=0, tiled=True),
        lax.all_gather(w_z, "sp", axis=0, tiled=True),
        lax.all_gather(w_b, "sp", axis=0, tiled=True),
        lax.all_gather(w_c, "sp", axis=0, tiled=True),
    )
    columns = normed
    pool_sum, x_sum, z_sum, b_sum, c_sum = tuple(
        (jnp.dot(columns, w_piece, preferred_element_type=jnp.float32) for w_piece in w_pieces)
    )
    pool_in = pool_sum.astype(jnp.bfloat16)
    ssd_x = x_sum.astype(jnp.bfloat16)
    gate_z = z_sum.astype(jnp.bfloat16)
    ssd_b = b_sum.astype(jnp.bfloat16)
    ssd_c = c_sum.astype(jnp.bfloat16)
    head_count = w_x.shape[1] // MIXER_HEAD_SIZE
    group_count = w_b.shape[1] // STATE
    per_group = head_count // group_count
    dt_raw = jnp.dot(
        normed, w_dt.reshape(w_dt.shape[0], 2 * head_count), preferred_element_type=jnp.float32
    ).reshape(tok_rows, 2, head_count)
    pool_width = pool_in.shape[1]
    conv_in = jnp.concatenate([ssd_x, ssd_b, ssd_c], axis=1)
    extended = with_halo(jnp.concatenate([pool_in, conv_in], axis=1), (("sp", 0),), pool_reach)
    pool_ext = extended[:, :pool_width]
    conv_ext = extended[pool_reach - 1 : pool_reach + tok_rows + 1, pool_width:]
    channel_group = (
        lax.axis_index("tp") * pool_width + jnp.arange(pool_width, dtype=jnp.int32)
    ) // POOL_GW
    first_pos = lax.axis_index("sp") * tok_rows
    seq_total = tok_rows * lax.axis_size("sp")
    pooled = (
        window_means(pool_ext.astype(jnp.float32), first_pos, seq_total, channel_group)
        - pool_in.astype(jnp.float32)
    ).astype(jnp.bfloat16)
    conv_weight = jnp.concatenate([conv_x, conv_b, output_map_taps], axis=1)
    convolved = rounded(conv_silu(conv_ext, conv_weight))
    x_width = w_x.shape[1]
    b_width = w_b.shape[1]
    heads_x = convolved[:, :x_width].reshape(tok_rows, group_count, per_group, MIXER_HEAD_SIZE)
    b_groups = convolved[:, x_width : x_width + b_width].reshape(tok_rows, group_count, STATE)
    c_groups = convolved[:, x_width + b_width :].reshape(tok_rows, group_count, STATE)
    step_size = jax.nn.softplus(dt_raw)
    log_decay = -step_size * jnp.exp(decay_log)[None] - leak
    step_size = step_size.reshape(tok_rows, 2, group_count, per_group)
    log_decay = log_decay.reshape(tok_rows, 2, group_count, per_group)
    start = init_state.reshape(2, group_count, per_group, MIXER_HEAD_SIZE, STATE)
    fwd_out, fwd_state, fwd_decay, fwd_cumul = nearby_orientation(
        heads_x, b_groups, c_groups, step_size[:, 0], log_decay[:, 0]
    )
    flip_x = heads_x[::-1]
    flip_b = b_groups[::-1]
    flip_c = c_groups[::-1]
    bwd_out, bwd_state, bwd_decay, bwd_cumul = nearby_orientation(
        flip_x, flip_b, flip_c, step_size[::-1, 1], log_decay[::-1, 1]
    )
    identity = (jnp.ones_like(fwd_decay), jnp.zeros_like(fwd_state))
    fwd_prefix = entering((fwd_decay, fwd_state), "sp", combine_states, identity, False)
    bwd_prefix = entering((bwd_decay, bwd_state), "sp", combine_states, identity, True)
    fwd_entry = fwd_prefix[1] + fwd_prefix[0][..., None, None] * start[0]
    bwd_entry = bwd_prefix[1] + bwd_prefix[0][..., None, None] * start[1]
    forward = including_element(fwd_out, c_groups, fwd_cumul, fwd_entry)
    backward = including_element(bwd_out, flip_c, bwd_cumul, bwd_entry)[::-1]
    gated = (forward + backward).reshape(tok_rows, head_count, MIXER_HEAD_SIZE) * jax.nn.silu(
        gate_z.astype(jnp.float32)
    ).reshape(tok_rows, head_count, MIXER_HEAD_SIZE)
    head_norm = gated * lax.rsqrt(jnp.mean(gated * gated, axis=2, keepdims=True) + epsilon)
    ssd_y = (head_norm.reshape(tok_rows, x_width) * head_gain.astype(jnp.float32)).astype(
        jnp.bfloat16
    )
    pooled_all, ssd_all = (
        lax.all_gather(pooled, "tp", axis=1, tiled=True),
        lax.all_gather(ssd_y, "tp", axis=1, tiled=True),
    )
    joined = jnp.concatenate([pooled_all, ssd_all], axis=1)
    columns = joined
    mixed = jnp.dot(
        columns, lax.all_gather(w_out, "sp", axis=0, tiled=True), preferred_element_type=jnp.float32
    )
    return mixed.astype(jnp.bfloat16)


def window_sums(values, channel_group):
    count = values.shape[0]
    reach = pool_reach
    padded = jnp.pad(values, ((reach, reach), (0, 0)))

    def shifted(array, offset):
        return jnp.roll(array, -offset, axis=0)

    sums = shifted(padded, -1) + padded
    chosen = sums
    half = 1
    for group_id in range(1, len(windows)):
        sums = shifted(sums, -half) + shifted(sums, half)
        half *= 2
        chosen = jnp.where(channel_group[None, :] >= group_id, sums, chosen)
    return chosen[reach : reach + count]


def pool_tokens(pool_in, channel_group):
    count = pool_in.shape[0]
    values = pool_in.astype(jnp.float32)
    position = jnp.arange(count, dtype=jnp.int32)[:, None]
    low = (jnp.asarray(windows, jnp.int32) // 2)[channel_group][None, :]
    high = (jnp.asarray(windows, jnp.int32) - 1)[channel_group][None, :] - low
    tallied = jnp.minimum(position + high, count - 1) - jnp.maximum(position - low, 0) + 1
    sums = window_sums(values, channel_group)
    return (sums / tallied.astype(jnp.float32) - values).astype(jnp.bfloat16)


def block_states(ends, own, start, reverse):
    count = ends.shape[0]
    index = jnp.arange(count)
    to, source, between = index[:, None, None], index[None, :, None], index[None, None, :]
    if reverse:
        to, source, between = -to, -source, -between
    inside = jnp.sum(
        jnp.where((source < between) & (between < to), ends[None, None, :], 0.0), axis=2
    )
    weights = jnp.exp(jnp.where(source[:, :, 0] < to[:, :, 0], inside, -jnp.inf))
    before = jnp.sum(jnp.where(between[0] < to[:, 0], ends[None, :], 0.0), axis=1)
    return (
        jnp.einsum("nm,mps->nps", weights, own, precision=lax.Precision.HIGHEST)
        + jnp.exp(before)[:, None, None] * start[None]
    )


def one_head(x_blk, b_blk, c_blk, step, decay, start):
    scores = jnp.einsum("nis,njs->nij", c_blk, b_blk, preferred_element_type=jnp.float32)
    index = jnp.arange(x_blk.shape[1])
    carried = 0.0
    factor = 0.0
    for direction in range(2):
        reverse = direction == 1
        cumul = lax.cumsum(decay[direction], axis=1, reverse=reverse)
        end = cumul[:, 0] if reverse else cumul[:, -1]
        visible = index[:, None] <= index[None, :] if reverse else index[:, None] >= index[None, :]
        gap = cumul[:, :, None] - cumul[:, None, :]
        factor = factor + (
            jnp.exp(jnp.where(visible[None], gap, -jnp.inf)) * step[direction][:, None, :]
        )
        to_end = jnp.exp(end[:, None] - cumul) * step[direction]
        scaled = (to_end[:, :, None] * b_blk.astype(jnp.float32)).astype(jnp.bfloat16)
        own = jnp.einsum("njp,njs->nps", x_blk, scaled, preferred_element_type=jnp.float32)
        states = block_states(end, own, start[direction], reverse)
        carried = carried + jnp.exp(cumul)[:, :, None] * jnp.einsum(
            "nis,nps->nip", c_blk.astype(jnp.float32), states, precision=lax.Precision.HIGHEST
        )
    mixing = (scores * factor).astype(jnp.bfloat16)
    inner = jnp.einsum("nij,njp->nip", mixing, x_blk, preferred_element_type=jnp.float32)
    return inner + carried


def head_per_device(
    tokens,
    norm_gain,
    w_pool_in,
    w_x,
    w_z,
    w_b,
    w_c,
    w_dt,
    conv_x,
    conv_b,
    output_map_taps,
    decay_log,
    leak,
    init_state,
    head_gain,
    w_out,
):
    spans = lax.axis_size("sp")
    span, side = lax.axis_index("sp"), lax.axis_index("tp")
    tok_rows, depth = tokens.shape[0], w_x.shape[0]
    seq_total = tok_rows * spans
    head_count = w_x.shape[1] // MIXER_HEAD_SIZE
    group_count = w_b.shape[1] // STATE
    per_group = head_count // group_count
    my_group = span // per_group
    pool_share = w_pool_in.shape[1] // spans
    sides = lax.axis_size("tp")

    part = tok_rows // sides
    token_f = lax.dynamic_slice_in_dim(tokens, side * part, part, 0).astype(jnp.float32)
    normed_part = (
        token_f
        * lax.rsqrt(jnp.mean(token_f * token_f, axis=1, keepdims=True) + epsilon)
        * norm_gain.astype(jnp.float32)
    ).astype(jnp.bfloat16)
    normed = lax.all_gather(normed_part, ("sp", "tp"), axis=0, tiled=True)

    def repeated(weight):
        groups = weight.reshape(depth, group_count, 1, STATE)
        return jnp.broadcast_to(groups, (depth, group_count, per_group, STATE)).reshape(
            depth, spans, STATE
        )

    packed = jnp.concatenate(
        [
            repeated(w_b),
            repeated(w_c),
            w_x.reshape(depth, spans, MIXER_HEAD_SIZE),
            w_z.reshape(depth, spans, MIXER_HEAD_SIZE),
            w_pool_in.reshape(depth, spans, pool_share),
        ],
        axis=2,
    )
    packed = jnp.transpose(packed, (1, 0, 2))
    moved = lax.all_to_all(packed, "sp", split_axis=0, concat_axis=0, tiled=True)
    weight = moved.reshape(depth * spans, packed.shape[2])
    w_step = lax.dynamic_slice_in_dim(w_dt, span, 1, 2)[:, :, 0]
    weight = jnp.concatenate([weight, w_step], axis=1)
    leak_all = lax.all_to_all(
        jnp.transpose(leak, (2, 1, 0)), "sp", split_axis=0, concat_axis=0, tiled=True
    )
    leak_mine = jnp.transpose(leak_all, (1, 0, 2))

    w_out, normed = lax.optimization_barrier((w_out, normed))
    w_out_all = lax.all_gather(w_out, "sp", axis=0, tiled=True)

    sums = jnp.dot(normed, weight, preferred_element_type=jnp.float32)
    width = 2 * STATE + MIXER_HEAD_SIZE
    conv_in = sums[:, :width].astype(jnp.bfloat16)
    gate_z = sums[:, width : width + MIXER_HEAD_SIZE].astype(jnp.bfloat16)
    pool_at = width + MIXER_HEAD_SIZE
    pool_in = sums[:, pool_at : pool_at + pool_share].astype(jnp.bfloat16)
    dt_raw = sums[:, pool_at + pool_share :]

    def own(array, size, at):
        return lax.dynamic_slice_in_dim(array, at * size, size, 1)

    taps = jnp.concatenate(
        [
            own(conv_b, STATE, my_group),
            own(output_map_taps, STATE, my_group),
            own(conv_x, MIXER_HEAD_SIZE, span),
        ],
        axis=1,
    )
    convolved = conv_silu(jnp.pad(conv_in, ((1, 1), (0, 0))), taps).astype(jnp.bfloat16)
    block_count = seq_total // BLOCK
    blocks = convolved.reshape(block_count, BLOCK, width)
    step = jax.nn.softplus(jnp.transpose(dt_raw)).reshape(2, block_count, BLOCK)
    rate = jnp.exp(own(decay_log, 1, span))[:, :, None]
    decay = -step * rate - leak_mine.reshape(2, block_count, BLOCK)
    start = lax.dynamic_index_in_dim(init_state, span, 1, keepdims=False)
    mixed_head = one_head(
        blocks[:, :, 2 * STATE :],
        blocks[:, :, :STATE],
        blocks[:, :, STATE : 2 * STATE],
        step,
        decay,
        start,
    ).reshape(seq_total, MIXER_HEAD_SIZE)
    gated = mixed_head * jax.nn.silu(gate_z.astype(jnp.float32))
    head_norm = gated * lax.rsqrt(jnp.mean(gated * gated, axis=1, keepdims=True) + epsilon)
    gain = lax.dynamic_slice_in_dim(head_gain, span * MIXER_HEAD_SIZE, MIXER_HEAD_SIZE, 0)
    ssd_y = (head_norm * gain.astype(jnp.float32)).astype(jnp.bfloat16)
    first = (side * spans + span) * pool_share
    channel_group = (first + jnp.arange(pool_share, dtype=jnp.int32)) // POOL_GW
    pooled = pool_tokens(pool_in, channel_group)

    mine = jnp.concatenate([pooled, ssd_y], axis=1).reshape(spans, tok_rows, -1)
    by_head = lax.all_to_all(mine, "sp", split_axis=0, concat_axis=0, tiled=True)
    everything = jnp.transpose(lax.all_gather(by_head, "tp", axis=0, tiled=True), (1, 0, 2))
    joined = jnp.concatenate(
        [
            everything[:, :, :pool_share].reshape(tok_rows, -1),
            everything[:, :, pool_share:].reshape(tok_rows, -1),
        ],
        axis=1,
    )
    mixed = jnp.dot(joined, w_out_all, preferred_element_type=jnp.float32)
    return mixed.astype(jnp.bfloat16)


def chosen_plan(*arguments):
    w_x, w_b = arguments[3], arguments[5]
    w_pool_in = arguments[2]
    spans, sides = lax.axis_size("sp"), lax.axis_size("tp")
    fits = (
        w_x.shape[1] == spans * MIXER_HEAD_SIZE
        and w_b.shape[1] % STATE == 0
        and w_pool_in.shape[1] % spans == 0
        and arguments[0].shape[0] % (8 * sides) == 0
    )
    return head_per_device(*arguments) if fits else per_device(*arguments)


def solution(mesh):
    return jax.shard_map(
        chosen_plan,
        mesh=mesh,
        in_specs=(
            P("sp", None),
            P(),
            P("sp", "tp"),
            P("sp", "tp"),
            P("sp", "tp"),
            P("sp", "tp"),
            P("sp", "tp"),
            P(None, None, "tp"),
            P(None, "tp"),
            P(None, "tp"),
            P(None, "tp"),
            P(None, "tp"),
            P("sp", None, "tp"),
            P(None, "tp", None, None),
            P("tp"),
            P("sp", "tp"),
        ),
        out_specs=P("sp", "tp"),
        check_vma=False,
    )
```

```python
import jax
import jax.numpy as jnp
from jax import lax
from jax.sharding import PartitionSpec as P

POOL_GW = 256
MIXER_HEAD_SIZE = 64
STATE = 128
BLOCK = 128


epsilon = 1e-06
windows = (2, 4, 8, 16)
pool_reach = 8


def with_halo(cells, sides, width):
    for axis, dim in sides:
        count = lax.axis_size(axis)
        ends = count - 1
        head = lax.slice_in_dim(cells, 0, width, axis=dim)
        tail = lax.slice_in_dim(cells, cells.shape[dim] - width, cells.shape[dim], axis=dim)
        cells = jnp.concatenate(
            [
                lax.ppermute(tail, axis, [(i, (i + 1) % count) for i in range(ends)]),
                cells,
                lax.ppermute(head, axis, [((i + 1) % count, i) for i in range(ends)]),
            ],
            axis=dim,
        )
    return cells


def entering(value, axis, combine, identity, reverse):
    length, mine = (lax.axis_size(axis), lax.axis_index(axis))
    everything = jax.tree.map(
        lambda part, kind: lax.all_gather(part.astype(kind), axis),
        value,
        (jnp.bfloat16, jnp.bfloat16),
    )
    start = jax.tree.map(
        lambda part, zero: jnp.broadcast_to(jnp.asarray(zero, part.dtype), part.shape),
        value,
        identity,
    )

    def lap(k, before):
        at = length - 1 - k if reverse else k
        reached = at > mine if reverse else at < mine
        new = combine(
            before, jax.tree.map(lambda part, own: part[at].astype(own.dtype), everything, value)
        )
        return jax.tree.map(lambda a, b: jnp.where(reached, a, b), new, before)

    return lax.fori_loop(0, length, lap, start)


def rounded(value):
    return lax.optimization_barrier(value.astype(jnp.bfloat16))


def window_means(padded, first_pos, seq_total, channel_group):
    count_rows = padded.shape[0] - 2 * pool_reach
    prefix = jnp.concatenate(
        [jnp.zeros((1, padded.shape[1]), jnp.float32), jnp.cumsum(padded, axis=0)], axis=0
    )
    element_index = first_pos + jnp.arange(count_rows, dtype=jnp.int32)
    result = jnp.zeros((count_rows, padded.shape[1]), jnp.float32)
    for group_id, window in enumerate(windows):
        low_reach = window // 2
        high_reach = window - 1 - low_reach
        upper_sum = prefix[pool_reach + high_reach + 1 : pool_reach + high_reach + 1 + count_rows]
        lower_sum = prefix[pool_reach - low_reach : pool_reach - low_reach + count_rows]
        tallied_items = (
            jnp.minimum(element_index + high_reach, seq_total - 1)
            - jnp.maximum(element_index - low_reach, 0)
            + 1
        )
        means = (upper_sum - lower_sum) / tallied_items.astype(jnp.float32)[:, None]
        result = jnp.where(channel_group[None, :] == group_id, means, result)
    return result


def conv_silu(extended, conv_weight):
    weight = conv_weight.astype(jnp.float32)
    values = extended.astype(jnp.float32)
    summed = values[:-2] * weight[0] + values[1:-1] * weight[1] + values[2:] * weight[2]
    return jax.nn.silu(summed)


def ssd_block(state_in, inputs):
    x_blk, b_blk, c_blk, dt_blk, decay_blk = inputs
    block_length = x_blk.shape[0]
    cumul = jnp.cumsum(decay_blk, axis=0)
    scores = jnp.einsum("ign,kgn->gik", c_blk, b_blk, preferred_element_type=jnp.float32)
    index = jnp.arange(block_length)
    below = index[:, None] >= index[None, :]
    cumul_t = jnp.transpose(cumul, (1, 2, 0))
    gap_log = cumul_t[:, :, :, None] - cumul_t[:, :, None, :]
    decay_mat = jnp.exp(jnp.where(below, gap_log, -jnp.inf))
    dt_t = jnp.transpose(dt_blk, (1, 2, 0))
    mixing = (scores[:, None] * decay_mat * dt_t[:, :, None, :]).astype(jnp.bfloat16)
    inner = jnp.einsum("gjik,kgjp->igjp", mixing, x_blk, preferred_element_type=jnp.float32)
    carried = jnp.exp(cumul)[..., None] * jnp.einsum(
        "ign,gjpn->igjp", c_blk.astype(jnp.float32), state_in, precision=lax.Precision.HIGHEST
    )
    to_end = jnp.exp(cumul[-1:] - cumul) * dt_blk
    scaled_b = (to_end[..., None] * b_blk.astype(jnp.float32)[:, :, None, :]).astype(jnp.bfloat16)
    state_out = jnp.exp(cumul[-1])[..., None, None] * state_in + jnp.einsum(
        "kgjp,kgjn->gjpn", x_blk, scaled_b, preferred_element_type=jnp.float32
    )
    return (state_out, inner + carried)


def nearby_orientation(heads_x, b_groups, c_groups, step_dir, decay_dir):
    block_count = heads_x.shape[0] // BLOCK

    def to_blocks(values_in):
        return values_in.reshape((block_count, BLOCK) + values_in.shape[1:])

    zero_state = jnp.zeros(
        (heads_x.shape[1], heads_x.shape[2], heads_x.shape[3], b_groups.shape[2]), jnp.float32
    )
    final_state, outputs = lax.scan(
        ssd_block,
        zero_state,
        (
            to_blocks(heads_x),
            to_blocks(b_groups),
            to_blocks(c_groups),
            to_blocks(step_dir),
            to_blocks(decay_dir),
        ),
    )
    cumul_span = jnp.cumsum(decay_dir, axis=0)
    return (outputs.reshape(heads_x.shape), final_state, jnp.exp(cumul_span[-1]), cumul_span)


def combine_states(earlier, later):
    return (earlier[0] * later[0], earlier[1] * later[0][..., None, None] + later[1])


def including_element(local_out, c_groups, cumul_span, entry):
    return local_out + jnp.exp(cumul_span)[..., None] * jnp.einsum(
        "tgn,gjpn->tgjp", c_groups.astype(jnp.float32), entry, precision=lax.Precision.HIGHEST
    )


def per_device(
    tokens,
    norm_gain,
    w_pool_in,
    w_x,
    w_z,
    w_b,
    w_c,
    w_dt,
    conv_x,
    conv_b,
    output_map_taps,
    decay_log,
    leak,
    init_state,
    head_gain,
    w_out,
):
    tok_rows = tokens.shape[0]
    token_f = tokens.astype(jnp.float32)
    normed = (
        token_f
        * lax.rsqrt(jnp.mean(token_f * token_f, axis=1, keepdims=True) + epsilon)
        * norm_gain.astype(jnp.float32)
    ).astype(jnp.bfloat16)
    w_pieces = (
        lax.all_gather(w_pool_in, "sp", axis=0, tiled=True),
        lax.all_gather(w_x, "sp", axis=0, tiled=True),
        lax.all_gather(w_z, "sp", axis=0, tiled=True),
        lax.all_gather(w_b, "sp", axis=0, tiled=True),
        lax.all_gather(w_c, "sp", axis=0, tiled=True),
    )
    columns = normed
    pool_sum, x_sum, z_sum, b_sum, c_sum = tuple(
        (jnp.dot(columns, w_piece, preferred_element_type=jnp.float32) for w_piece in w_pieces)
    )
    pool_in = pool_sum.astype(jnp.bfloat16)
    ssd_x = x_sum.astype(jnp.bfloat16)
    gate_z = z_sum.astype(jnp.bfloat16)
    ssd_b = b_sum.astype(jnp.bfloat16)
    ssd_c = c_sum.astype(jnp.bfloat16)
    head_count = w_x.shape[1] // MIXER_HEAD_SIZE
    group_count = w_b.shape[1] // STATE
    per_group = head_count // group_count
    dt_raw = jnp.dot(
        normed, w_dt.reshape(w_dt.shape[0], 2 * head_count), preferred_element_type=jnp.float32
    ).reshape(tok_rows, 2, head_count)
    pool_width = pool_in.shape[1]
    conv_in = jnp.concatenate([ssd_x, ssd_b, ssd_c], axis=1)
    extended = with_halo(jnp.concatenate([pool_in, conv_in], axis=1), (("sp", 0),), pool_reach)
    pool_ext = extended[:, :pool_width]
    conv_ext = extended[pool_reach - 1 : pool_reach + tok_rows + 1, pool_width:]
    channel_group = (
        lax.axis_index("tp") * pool_width + jnp.arange(pool_width, dtype=jnp.int32)
    ) // POOL_GW
    first_pos = lax.axis_index("sp") * tok_rows
    seq_total = tok_rows * lax.axis_size("sp")
    pooled = (
        window_means(pool_ext.astype(jnp.float32), first_pos, seq_total, channel_group)
        - pool_in.astype(jnp.float32)
    ).astype(jnp.bfloat16)
    conv_weight = jnp.concatenate([conv_x, conv_b, output_map_taps], axis=1)
    convolved = rounded(conv_silu(conv_ext, conv_weight))
    x_width = w_x.shape[1]
    b_width = w_b.shape[1]
    heads_x = convolved[:, :x_width].reshape(tok_rows, group_count, per_group, MIXER_HEAD_SIZE)
    b_groups = convolved[:, x_width : x_width + b_width].reshape(tok_rows, group_count, STATE)
    c_groups = convolved[:, x_width + b_width :].reshape(tok_rows, group_count, STATE)
    step_size = jax.nn.softplus(dt_raw)
    log_decay = -step_size * jnp.exp(decay_log)[None] - leak
    step_size = step_size.reshape(tok_rows, 2, group_count, per_group)
    log_decay = log_decay.reshape(tok_rows, 2, group_count, per_group)
    start = init_state.reshape(2, group_count, per_group, MIXER_HEAD_SIZE, STATE)
    fwd_out, fwd_state, fwd_decay, fwd_cumul = nearby_orientation(
        heads_x, b_groups, c_groups, step_size[:, 0], log_decay[:, 0]
    )
    flip_x = heads_x[::-1]
    flip_b = b_groups[::-1]
    flip_c = c_groups[::-1]
    bwd_out, bwd_state, bwd_decay, bwd_cumul = nearby_orientation(
        flip_x, flip_b, flip_c, step_size[::-1, 1], log_decay[::-1, 1]
    )
    identity = (jnp.ones_like(fwd_decay), jnp.zeros_like(fwd_state))
    fwd_prefix = entering((fwd_decay, fwd_state), "sp", combine_states, identity, False)
    bwd_prefix = entering((bwd_decay, bwd_state), "sp", combine_states, identity, True)
    fwd_entry = fwd_prefix[1] + fwd_prefix[0][..., None, None] * start[0]
    bwd_entry = bwd_prefix[1] + bwd_prefix[0][..., None, None] * start[1]
    forward = including_element(fwd_out, c_groups, fwd_cumul, fwd_entry)
    backward = including_element(bwd_out, flip_c, bwd_cumul, bwd_entry)[::-1]
    gated = (forward + backward).reshape(tok_rows, head_count, MIXER_HEAD_SIZE) * jax.nn.silu(
        gate_z.astype(jnp.float32)
    ).reshape(tok_rows, head_count, MIXER_HEAD_SIZE)
    head_norm = gated * lax.rsqrt(jnp.mean(gated * gated, axis=2, keepdims=True) + epsilon)
    ssd_y = (head_norm.reshape(tok_rows, x_width) * head_gain.astype(jnp.float32)).astype(
        jnp.bfloat16
    )
    pooled_all, ssd_all = (
        lax.all_gather(pooled, "tp", axis=1, tiled=True),
        lax.all_gather(ssd_y, "tp", axis=1, tiled=True),
    )
    joined = jnp.concatenate([pooled_all, ssd_all], axis=1)
    columns = joined
    mixed = jnp.dot(
        columns, lax.all_gather(w_out, "sp", axis=0, tiled=True), preferred_element_type=jnp.float32
    )
    return mixed.astype(jnp.bfloat16)


def window_sums(values, channel_group):
    count = values.shape[0]
    reach = pool_reach
    padded = jnp.pad(values, ((reach, reach), (0, 0)))

    def shifted(array, offset):
        return jnp.roll(array, -offset, axis=0)

    sums = shifted(padded, -1) + padded
    chosen = sums
    half = 1
    for group_id in range(1, len(windows)):
        sums = shifted(sums, -half) + shifted(sums, half)
        half *= 2
        chosen = jnp.where(channel_group[None, :] >= group_id, sums, chosen)
    return chosen[reach : reach + count]


def pool_tokens(pool_in, channel_group):
    count = pool_in.shape[0]
    values = pool_in.astype(jnp.float32)
    position = jnp.arange(count, dtype=jnp.int32)[:, None]
    low = (jnp.asarray(windows, jnp.int32) // 2)[channel_group][None, :]
    high = (jnp.asarray(windows, jnp.int32) - 1)[channel_group][None, :] - low
    tallied = jnp.minimum(position + high, count - 1) - jnp.maximum(position - low, 0) + 1
    sums = window_sums(values, channel_group)
    return (sums / tallied.astype(jnp.float32) - values).astype(jnp.bfloat16)


def block_states(ends, own, start, reverse):
    count = ends.shape[0]
    index = jnp.arange(count)
    to, source, between = index[:, None, None], index[None, :, None], index[None, None, :]
    if reverse:
        to, source, between = -to, -source, -between
    inside = jnp.sum(
        jnp.where((source < between) & (between < to), ends[None, None, :], 0.0), axis=2
    )
    weights = jnp.exp(jnp.where(source[:, :, 0] < to[:, :, 0], inside, -jnp.inf))
    before = jnp.sum(jnp.where(between[0] < to[:, 0], ends[None, :], 0.0), axis=1)
    return (
        jnp.einsum("nm,mps->nps", weights, own, precision=lax.Precision.HIGHEST)
        + jnp.exp(before)[:, None, None] * start[None]
    )


def one_head(x_blk, b_blk, c_blk, step, decay, start):
    scores = jnp.einsum("nis,njs->nij", c_blk, b_blk, preferred_element_type=jnp.float32)
    index = jnp.arange(x_blk.shape[1])
    carried = 0.0
    factor = 0.0
    for direction in range(2):
        reverse = direction == 1
        cumul = lax.cumsum(decay[direction], axis=1, reverse=reverse)
        end = cumul[:, 0] if reverse else cumul[:, -1]
        visible = index[:, None] <= index[None, :] if reverse else index[:, None] >= index[None, :]
        gap = cumul[:, :, None] - cumul[:, None, :]
        factor = factor + (
            jnp.exp(jnp.where(visible[None], gap, -jnp.inf)) * step[direction][:, None, :]
        )
        to_end = jnp.exp(end[:, None] - cumul) * step[direction]
        scaled = (to_end[:, :, None] * b_blk.astype(jnp.float32)).astype(jnp.bfloat16)
        own = jnp.einsum("njp,njs->nps", x_blk, scaled, preferred_element_type=jnp.float32)
        states = block_states(end, own, start[direction], reverse)
        carried = carried + jnp.exp(cumul)[:, :, None] * jnp.einsum(
            "nis,nps->nip", c_blk.astype(jnp.float32), states, precision=lax.Precision.HIGHEST
        )
    mixing = (scores * factor).astype(jnp.bfloat16)
    inner = jnp.einsum("nij,njp->nip", mixing, x_blk, preferred_element_type=jnp.float32)
    return inner + carried


leak_parts = 3


def leak_columns(leak, depth):
    rest = jnp.transpose(leak, (2, 1, 0))
    parts = []
    for _ in range(leak_parts):
        part = rounded(rest)
        parts.append(part)
        rest = rest - part.astype(jnp.float32)
    sent = jnp.stack(parts, axis=1).reshape(rest.shape[0], -1, depth)
    return jnp.transpose(sent, (0, 2, 1))


def head_per_device(
    tokens,
    norm_gain,
    w_pool_in,
    w_x,
    w_z,
    w_b,
    w_c,
    w_dt,
    conv_x,
    conv_b,
    output_map_taps,
    decay_log,
    leak,
    init_state,
    head_gain,
    w_out,
):
    spans = lax.axis_size("sp")
    span, side = lax.axis_index("sp"), lax.axis_index("tp")
    tok_rows, depth = tokens.shape[0], w_x.shape[0]
    seq_total = tok_rows * spans
    head_count = w_x.shape[1] // MIXER_HEAD_SIZE
    group_count = w_b.shape[1] // STATE
    per_group = head_count // group_count
    my_group = span // per_group
    pool_share = w_pool_in.shape[1] // spans
    sides = lax.axis_size("tp")

    part = tok_rows // sides
    token_f = lax.dynamic_slice_in_dim(tokens, side * part, part, 0).astype(jnp.float32)
    normed_part = (
        token_f
        * lax.rsqrt(jnp.mean(token_f * token_f, axis=1, keepdims=True) + epsilon)
        * norm_gain.astype(jnp.float32)
    ).astype(jnp.bfloat16)
    normed = lax.all_gather(normed_part, ("sp", "tp"), axis=0, tiled=True)

    def repeated(weight):
        groups = weight.reshape(depth, group_count, 1, STATE)
        return jnp.broadcast_to(groups, (depth, group_count, per_group, STATE)).reshape(
            depth, spans, STATE
        )

    packed = jnp.concatenate(
        [
            repeated(w_b),
            repeated(w_c),
            w_x.reshape(depth, spans, MIXER_HEAD_SIZE),
            w_z.reshape(depth, spans, MIXER_HEAD_SIZE),
            w_pool_in.reshape(depth, spans, pool_share),
        ],
        axis=2,
    )
    packed = jnp.concatenate(
        [jnp.transpose(packed, (1, 0, 2)), leak_columns(leak, depth)], axis=2
    )
    moved = lax.all_to_all(packed, "sp", split_axis=0, concat_axis=0, tiled=True)
    w_out, normed, moved = lax.optimization_barrier((w_out, normed, moved))
    w_out_all = lax.all_gather(w_out, "sp", axis=0, tiled=True)
    weight = moved.reshape(depth * spans, packed.shape[2])
    w_step = lax.dynamic_slice_in_dim(w_dt, span, 1, 2)[:, :, 0]
    weight = jnp.concatenate([weight, w_step], axis=1)
    parts_at = packed.shape[2] - leak_parts * 2 * tok_rows // depth
    leak_sent = moved.reshape(spans, depth, packed.shape[2])[:, :, parts_at:]
    leak_sent = jnp.transpose(leak_sent, (0, 2, 1)).reshape(spans, leak_parts, 2, tok_rows)
    leak_mine = jnp.transpose(
        jnp.sum(leak_sent.astype(jnp.float32)[:, ::-1], axis=1), (1, 0, 2)
    )

    sums = jnp.dot(normed, weight, preferred_element_type=jnp.float32)
    width = 2 * STATE + MIXER_HEAD_SIZE
    conv_in = sums[:, :width].astype(jnp.bfloat16)
    gate_z = sums[:, width : width + MIXER_HEAD_SIZE].astype(jnp.bfloat16)
    pool_at = width + MIXER_HEAD_SIZE
    pool_in = sums[:, pool_at : pool_at + pool_share].astype(jnp.bfloat16)
    dt_raw = sums[:, packed.shape[2] :]

    def own(array, size, at):
        return lax.dynamic_slice_in_dim(array, at * size, size, 1)

    taps = jnp.concatenate(
        [
            own(conv_b, STATE, my_group),
            own(output_map_taps, STATE, my_group),
            own(conv_x, MIXER_HEAD_SIZE, span),
        ],
        axis=1,
    )
    convolved = conv_silu(jnp.pad(conv_in, ((1, 1), (0, 0))), taps).astype(jnp.bfloat16)
    block_count = seq_total // BLOCK
    blocks = convolved.reshape(block_count, BLOCK, width)
    step = jax.nn.softplus(jnp.transpose(dt_raw)).reshape(2, block_count, BLOCK)
    rate = jnp.exp(own(decay_log, 1, span))[:, :, None]
    decay = -step * rate - leak_mine.reshape(2, block_count, BLOCK)
    start = lax.dynamic_index_in_dim(init_state, span, 1, keepdims=False)
    mixed_head = one_head(
        blocks[:, :, 2 * STATE :],
        blocks[:, :, :STATE],
        blocks[:, :, STATE : 2 * STATE],
        step,
        decay,
        start,
    ).reshape(seq_total, MIXER_HEAD_SIZE)
    gated = mixed_head * jax.nn.silu(gate_z.astype(jnp.float32))
    head_norm = gated * lax.rsqrt(jnp.mean(gated * gated, axis=1, keepdims=True) + epsilon)
    gain = lax.dynamic_slice_in_dim(head_gain, span * MIXER_HEAD_SIZE, MIXER_HEAD_SIZE, 0)
    ssd_y = (head_norm * gain.astype(jnp.float32)).astype(jnp.bfloat16)
    first = (side * spans + span) * pool_share
    channel_group = (first + jnp.arange(pool_share, dtype=jnp.int32)) // POOL_GW
    pooled = pool_tokens(pool_in, channel_group)

    mine = jnp.concatenate([pooled, ssd_y], axis=1).reshape(spans, tok_rows, -1)
    by_head = lax.all_to_all(mine, "sp", split_axis=0, concat_axis=0, tiled=True)
    everything = jnp.transpose(lax.all_gather(by_head, "tp", axis=0, tiled=True), (1, 0, 2))
    joined = jnp.concatenate(
        [
            everything[:, :, :pool_share].reshape(tok_rows, -1),
            everything[:, :, pool_share:].reshape(tok_rows, -1),
        ],
        axis=1,
    )
    mixed = jnp.dot(joined, w_out_all, preferred_element_type=jnp.float32)
    return mixed.astype(jnp.bfloat16)


def chosen_plan(*arguments):
    w_x, w_b = arguments[3], arguments[5]
    w_pool_in = arguments[2]
    spans, sides = lax.axis_size("sp"), lax.axis_size("tp")
    fits = (
        w_x.shape[1] == spans * MIXER_HEAD_SIZE
        and w_b.shape[1] % STATE == 0
        and w_pool_in.shape[1] % spans == 0
        and arguments[0].shape[0] % (8 * sides) == 0
        and leak_parts * 2 * arguments[0].shape[0] % w_x.shape[0] == 0
    )
    return head_per_device(*arguments) if fits else per_device(*arguments)


def solution(mesh):
    return jax.shard_map(
        chosen_plan,
        mesh=mesh,
        in_specs=(
            P("sp", None),
            P(),
            P("sp", "tp"),
            P("sp", "tp"),
            P("sp", "tp"),
            P("sp", "tp"),
            P("sp", "tp"),
            P(None, None, "tp"),
            P(None, "tp"),
            P(None, "tp"),
            P(None, "tp"),
            P(None, "tp"),
            P("sp", None, "tp"),
            P(None, "tp", None, None),
            P("tp"),
            P("sp", "tp"),
        ),
        out_specs=P("sp", "tp"),
        check_vma=False,
    )
```
